32 devices in a mesh: grp: 2 (over x), ep: 8 (over z, y), tp: 2 (over core).
Axes of the slice: x: 2, y: 2, z: 4, core: 2. Of those that a mesh axis runs over, the one named last changes fastest.
Arguments:
- tokens: bfloat16 [128, 1536], P(('grp', 'ep')), parts along dimension 0, may hold values from -6 to 6
- norm_gain: float32 [1536], replicated, may hold values from 0.1 to 1.9
- routes: int32 [128, 4], P(('grp', 'ep')), parts along dimension 0, may hold values from 0 to 7, all different within a row; in each aligned block of 8 rows (0 to 7, 8 to 15, ...) at most 8 rows name the same one
- route_weight: float32 [128, 4], P(('grp', 'ep')), parts along dimension 0, may hold values from 0.1 to 1
- expert_gate: bfloat16 [8, 1536, 1536], P('ep', None, 'tp'), may hold values from -2 to 2
- expert_up: bfloat16 [8, 1536, 1536], P('ep', None, 'tp'), may hold values from -2 to 2
- expert_down: bfloat16 [8, 1536, 1536], P('ep', 'tp'), may hold values from -0.0390625 to 0.0390625
- dense_gate: bfloat16 [1536, 4096], P(None, ('ep', 'tp')), may hold values from -2 to 2
- dense_up: bfloat16 [1536, 4096], P(None, ('ep', 'tp')), may hold values from -2 to 2
- dense_down: bfloat16 [4096, 1536], P(('ep', 'tp')), may hold values from -0.0234375 to 0.0234375
- gate_vector: bfloat16 [4096], P(('ep', 'tp')), may hold values from -0.0234375 to 0.0234375
Outputs:
- mixed: bfloat16 [128, 1536], P(('grp', 'ep'), 'tp'), parts along dimension 0
The draws below stay inside these ranges and needn't reach their ends.
There are 2 independent parts, one for each index of `grp`. The reference program is written for one: setup_inputs(seed, part) draws one part's arguments, and reference() takes and returns one part's arrays. A program takes and returns all parts, laid end to end along the dimension named above; an argument that names none is the same for every part. Nothing has to cross between parts.
Inputs may be any that keep to these rules, and one draw needn't show every extreme that they name: `routes`: each token names 4 different experts. Within the rows of one index of ep (aligned blocks of 8 rows) no expert is named by more than 8 rows, a bound that some block reaches.
All inputs are finite; a program needn't handle non-finite values.
Results may differ from the reference program's by a relative error of at most 0.0077.
Values may be sent and summed in bfloat16 or wider, within the bound.
A program may use at most 64 MiB of HBM per device.

```python
import math
import jax
import jax.numpy as jnp
import numpy as np
from jax import lax

D = 1536
F = 1536
SH = 4096
TOPK = 4
TOK_DEV = 8
EXPERTS = 8
TOKENS = 64
CAP = 8
N_EP = 8
N_TP = 2


def scaled_weight(key, array_shape, fan_in):
    key_base, key_scale = jax.random.split(key)
    normals = jnp.clip(jax.random.normal(key_base, array_shape, jnp.float32), -5.0, 5.0)
    scale_shape = array_shape[:-2] + (1, array_shape[-1])
    low_end, high_end = (1.0, 3.0)
    column_scale = jnp.exp(jax.random.uniform(key_scale, scale_shape, jnp.float32, jnp.log(low_end), jnp.log(high_end)))
    values = jnp.clip(normals * column_scale * fan_in ** (-0.5), -2.0, 2.0)
    return values.astype(jnp.bfloat16)


def draw_expert_gate(key, part):
    return scaled_weight(jax.random.fold_in(key, 11), (EXPERTS, D, F), D)


def draw_expert_up(key, part):
    return scaled_weight(jax.random.fold_in(key, 23), (EXPERTS, D, F), D)


def draw_dense_gate(key, part):
    return scaled_weight(jax.random.fold_in(key, 37), (D, SH), D)


def draw_dense_up(key, part):
    return scaled_weight(jax.random.fold_in(key, 41), (D, SH), D)


def shard_levels(rng, dims, cuts, low, largest):
    loudness, own = 1.0, jax.random.fold_in(rng, 6)
    for position, parts in cuts:
        steps = jnp.exp(jax.random.uniform(jax.random.fold_in(own, position), (parts,), jnp.float32, low / len(cuts), largest / len(cuts)))
        loudness = loudness * jnp.repeat(steps, dims[position] // parts).reshape([-1 if axis == position else 1 for axis in range(len(dims))])
    return loudness


def deal_out(key, own, number, rows, amount, top, reach, skew):
    sequence = jax.random.permutation(key, amount)
    packed, ordinary = shares(amount, rows * top, reach, skew, True), shares(amount, rows * top, reach, skew, False)
    places = jnp.arange(amount)

    def named(tallies, offset_by):
        used = int((tallies > 0).sum())
        fixed = max(1, used // 4)
        passed = fixed + (places - fixed + offset_by * (used - fixed)) % max(1, amount - fixed)
        return jnp.zeros((amount,), jnp.int32).at[sequence[jnp.where(places < fixed, places, passed)]].set(jnp.asarray(tallies, jnp.int32))

    tallies = jnp.where(number % 4 == 0, named(packed, number // 4), named(ordinary, number - number // 4 - 1))
    mixed = jax.random.permutation(jax.random.fold_in(own, 3), amount)
    source_of, receiver = mixed[0:amount // 2 * 2:2], mixed[1:amount // 2 * 2:2]
    slack = jnp.minimum(tallies[source_of] - 1, reach - tallies[receiver]) // 2
    slack = jnp.where((source_of == sequence[0]) | (receiver == sequence[0]) | (tallies[receiver] == 0), 0, jnp.maximum(slack, 0))
    passed = jax.random.randint(jax.random.fold_in(own, 4), (amount // 2,), 0, 1 << 20) % (slack + 1)
    tallies = tallies.at[source_of].add(-passed).at[receiver].add(passed)
    labels = jnp.searchsorted(jnp.cumsum(tallies), jnp.arange(rows * top), side="right").astype(jnp.int32)
    listing = labels.reshape(top, rows).T
    listing = listing[jax.random.permutation(jax.random.fold_in(own, 1), rows)]
    offset_by = jax.random.randint(jax.random.fold_in(own, 2), (rows, 1), 0, top)
    return jnp.take_along_axis(listing, (jnp.arange(top)[None, :] + offset_by) % top, axis=1)


def shares(number_of, total, most, skew, full):
    portions = [(1 << 20) // math.isqrt(grade ** skew) + 1 for grade in range(1, number_of + 1)]
    largest = most if full else min(most, max(-(-total // number_of), total * portions[0] // sum(portions)))
    least = 1 if total - largest >= number_of - 1 else 0
    given, rest = [largest] + [least] * (number_of - 1), total - largest - least * (number_of - 1)
    while rest > 0:
        free = [i for i in range(1, number_of) if given[i] < largest] or [i for i in range(1, number_of) if given[i] < most]
        whole, budget = sum([portions[i] for i in free]), rest
        for i in free:
            more = min(most - given[i], max(1, budget * portions[i] // whole), rest)
            given[i] = given[i] + more
            rest = rest - more
    return np.array(given)


def normal_values(key, extent, scale, limit, shards=(), kind=jnp.bfloat16):
    values = jax.random.normal(key, extent, jnp.float32) * scale
    if len(shards) > 0:
        values = shard_levels(key, extent, shards, -0.22, 0.18) * values
    return jnp.clip(values, min=-limit, max=limit).astype(kind)


def setup_inputs(seed: int = 0, part: int = 0) -> dict:
    keys = jax.random.split(jax.random.key(seed), 12)
    part_keys = jax.random.split(jax.random.fold_in(keys[11], part), 12)
    tokens = normal_values(part_keys[0], (TOKENS, D), 1.0, 6.0, ((0, 8),))
    norm_gain = jnp.clip(1.0 + 0.18 * jax.random.normal(keys[1], (D,), jnp.float32), 0.1, 1.9)
    routes_keys = jax.random.split(jax.random.fold_in(part_keys[2], 1), TOKENS // TOK_DEV)
    routes_turns = jax.random.permutation(jax.random.fold_in(part_keys[2], 3), TOKENS // TOK_DEV)
    routes = jax.vmap(lambda own, number: deal_out(jax.random.fold_in(part_keys[2], 2), own, number, TOK_DEV, EXPERTS, TOPK, CAP, 2))(routes_keys, routes_turns).reshape((TOKENS, TOPK))
    route_weight = jnp.clip(jnp.exp(math.log(1.0) - 2.3025851 * jax.random.uniform(part_keys[3], (TOKENS, TOPK), jnp.float32) ** shard_levels(part_keys[3], (TOKENS, TOPK), ((0, 8),), -0.2, 0.2)), 0.1, 1.0)
    expert_gate = draw_expert_gate(jax.random.fold_in(keys[11], 71), part)
    expert_up = draw_expert_up(jax.random.fold_in(keys[11], 71), part)
    expert_down = normal_values(keys[6], (EXPERTS, F, D), (16 * F) ** -0.5, 0.0390625, ((0, 8), (1, 2)))
    dense_gate = draw_dense_gate(jax.random.fold_in(keys[11], 71), part)
    dense_up = draw_dense_up(jax.random.fold_in(keys[11], 71), part)
    dense_down = normal_values(keys[9], (SH, D), (16 * SH) ** -0.5, 0.0234375, ((0, 16),))
    gate_vector = normal_values(keys[10], (SH,), (16 * SH) ** -0.5, 0.0234375, ((0, 16),))
    return {"tokens": tokens, "norm_gain": norm_gain, "routes": routes, "route_weight": route_weight, "expert_gate": expert_gate, "expert_up": expert_up, "expert_down": expert_down, "dense_gate": dense_gate, "dense_up": dense_up, "dense_down": dense_down, "gate_vector": gate_vector}


clamp_limit = 7.0
sigmoid_slope = 1.702
norm_eps = 1e-06

def clamped_unit(gate_pre, up_pre):
    gated = jnp.minimum(gate_pre, clamp_limit)
    linear = jnp.clip(up_pre, -clamp_limit, clamp_limit)
    return (gated * jax.nn.sigmoid(sigmoid_slope * gated) * (linear + 1.0)).astype(jnp.bfloat16)

def rms_normed(tokens, norm_gain):
    values = tokens.astype(jnp.float32)
    inverse = lax.rsqrt(lax.optimization_barrier(jnp.mean(values * values, axis=-1, keepdims=True)) + norm_eps)
    return (values * inverse * norm_gain).astype(jnp.bfloat16)

def reference(tokens, norm_gain, routes, route_weight, expert_gate, expert_up, expert_down, dense_gate, dense_up, dense_down, gate_vector):
    normed = rms_normed(tokens, norm_gain)
    hidden = clamped_unit(jnp.dot(normed, dense_gate, preferred_element_type=jnp.float32), jnp.dot(normed, dense_up, preferred_element_type=jnp.float32))
    gate_logit = jnp.dot(hidden, gate_vector, preferred_element_type=jnp.float32)
    dense_out = jnp.dot(hidden, dense_down, preferred_element_type=jnp.float32)
    padded = jnp.concatenate([normed, jnp.zeros((1, D), jnp.bfloat16)], axis=0)
    half_width = F // N_TP

    def one_expert(totals, expert):
        matches = routes == expert
        chosen = jnp.any(matches, axis=1)
        weight = lax.optimization_barrier(jnp.sum(jnp.where(matches, route_weight, jnp.zeros_like(route_weight)), axis=1))
        weight = jnp.concatenate([weight, jnp.zeros((1,), weight.dtype)], axis=0)
        row_index = jnp.nonzero(chosen, size=N_EP * CAP, fill_value=TOKENS)[0].astype(jnp.int32)
        row_values = padded[row_index]
        expert_act = clamped_unit(jnp.dot(row_values, expert_gate[expert], preferred_element_type=jnp.float32), jnp.dot(row_values, expert_up[expert], preferred_element_type=jnp.float32))
        down_rows = expert_down[expert]
        outputs = jnp.zeros((row_values.shape[0], D), jnp.float32)
        for part_index in range(N_TP):
            pieces = jnp.dot(expert_act[:, part_index * half_width:(part_index + 1) * half_width], down_rows[part_index * half_width:(part_index + 1) * half_width], preferred_element_type=jnp.float32)
            outputs = outputs + lax.optimization_barrier(pieces.astype(jnp.bfloat16)).astype(jnp.float32)
        outputs = lax.optimization_barrier(outputs.astype(jnp.bfloat16)).astype(jnp.float32)
        totals = totals.at[row_index].add(weight[row_index][:, None] * outputs)
        return (totals, None)
    totals, _ = lax.scan(one_expert, jnp.zeros((TOKENS + 1, D), jnp.float32), jnp.arange(EXPERTS, dtype=jnp.int32))
    expert_mix = totals[:TOKENS]
    mixed = jax.nn.sigmoid(gate_logit)[:, None] * dense_out + expert_mix
    return mixed.astype(jnp.bfloat16)
```

```python
import functools

import jax
import jax.numpy as jnp
from jax import lax
from jax.experimental import pallas as pl
from jax.experimental.pallas import tpu as pltpu
from jax.sharding import PartitionSpec as P

MESH = pl.DeviceIdType.MESH
F32 = jnp.float32
BF16 = jnp.bfloat16
clamp_limit = 7.0
sigmoid_slope = 1.702
norm_eps = 1e-06
vmem_bytes = 67043328
extra = 128


def clamped_unit(gate_pre, up_pre):
    gated = jnp.minimum(gate_pre, clamp_limit)
    linear = jnp.clip(up_pre, -clamp_limit, clamp_limit)
    return (gated * jax.nn.sigmoid(sigmoid_slope * gated) * (linear + 1.0)).astype(BF16)


def split_lanes(value, shape):
    high = value.astype(BF16).astype(F32)
    middle = (value - high).astype(BF16).astype(F32)
    low = value - high - middle
    lane = lax.broadcasted_iota(jnp.int32, shape, len(shape) - 1)
    zero = jnp.zeros(shape, F32)
    out = jnp.where(lane == 0, high, jnp.where(lane == 1, middle, jnp.where(lane == 2, low, zero)))
    return out.astype(BF16)


def kernel(
    n, step,
    tok_hbm, gain_hbm, routes_hbm, weight_hbm, eg_hbm, eu_hbm, ed_hbm, dg_hbm, du_hbm, dd_hbm, gv_hbm,
    out_ref,
    tok, gain, routes, weight, gv, eg, eu, ed, dg, du, dd,
    x_mine, x_mate, acc_g, acc_u, acc_dg, acc_du, act, hidden, d_keep, e_keep, logit,
    d_give, d_take, d_out, d_in, e_give, e_take, e_out, e_in,
    small_sem, load_sem, x_send, x_recv, f_send, f_recv, d_send, d_recv, e_send, e_recv, p_send, p_recv,
):
    me, core = lax.axis_index("ep"), lax.axis_index("tp")
    mate = 1 - core
    rows, half = tok.shape[0], x_mine.shape[2]

    def peers(body):
        if n <= 16:
            order = sorted(range(1, n), key=lambda off: (abs(off - n + 2) % (n - 2), off))
            for off in order:
                body(lax.rem(me + off, n))
        else:
            def one(off, carry):
                body(lax.rem(me + off, n))
                return carry
            lax.fori_loop(1, n, one, 0)

    def chunks(body):
        if step == n:
            body(0)
        else:
            def one(index, carry):
                body(index * step)
                return carry
            lax.fori_loop(0, n // step, one, 0)

    def send(src, dst, ssem, rsem, device):
        return pltpu.make_async_remote_copy(
            src_ref=src, dst_ref=dst, send_sem=ssem, recv_sem=rsem,
            device_id=device, device_id_type=MESH,
        )

    barrier = pltpu.get_barrier_semaphore()
    peers(lambda p: pl.semaphore_signal(barrier, inc=1, device_id={"ep": p}, device_id_type=MESH))
    pl.semaphore_signal(barrier, inc=1, device_id={"tp": mate}, device_id_type=MESH)

    small = [
        pltpu.make_async_copy(src, dst, small_sem.at[i])
        for i, (src, dst) in enumerate(
            ((tok_hbm, tok), (gain_hbm, gain), (routes_hbm, routes), (weight_hbm, weight), (gv_hbm, gv))
        )
    ]
    for copy in small:
        copy.start()
    sides = (core, mate)
    loads = {}
    count = 0
    for name, src, dst, along in (
        ("dg", dg_hbm, dg, 0), ("du", du_hbm, du, 0), ("eg", eg_hbm.at[0], eg, 0),
        ("eu", eu_hbm.at[0], eu, 0), ("dd", dd_hbm, dd, 1), ("ed", ed_hbm.at[0], ed, 1),
    ):
        for k in range(2):
            cut = pl.ds(pl.multiple_of(sides[k] * half, 128), half)
            part = src.at[cut, :] if along == 0 else src.at[:, cut]
            loads[name, k] = pltpu.make_async_copy(part, dst.at[k], load_sem.at[count])
            count += 1
    for key in (("dg", 0), ("du", 0), ("eg", 0), ("eu", 0), ("dg", 1), ("du", 1), ("dd", 1), ("dd", 0),
                ("eg", 1), ("eu", 1), ("ed", 1), ("ed", 0)):
        loads[key].start()

    small[0].wait()
    small[1].wait()
    values = tok[...].astype(F32)
    inverse = lax.rsqrt(jnp.mean(values * values, axis=-1, keepdims=True) + norm_eps)
    normed = values * inverse * gain[...].reshape(1, 2 * half)
    left, right = normed[:, :half], normed[:, half:]
    first = core == 0
    x_mine[me] = jnp.where(first, left, right).astype(BF16)
    x_mate[me] = jnp.where(first, right, left).astype(BF16)

    pl.semaphore_wait(barrier, n)
    peers(lambda p: send(x_mine.at[me], x_mine.at[me], x_send.at[p], x_recv.at[me], {"ep": p}).start())

    def forward(p):
        send(x_mine.at[p], x_mine.at[p], x_send.at[p], x_recv.at[p], {"ep": p}).wait_recv()
        send(x_mine.at[p], x_mate.at[p], f_send.at[p], f_recv.at[p], {"tp": mate}).start()

    peers(forward)

    def at(ref, start):
        return pl.ds(start * rows, step * rows)

    def dot(a, b):
        return jnp.dot(a, b, preferred_element_type=F32)

    for key in (("dg", 0), ("du", 0), ("eg", 0), ("eu", 0)):
        loads[key].wait()

    def first_half(start):
        x = x_mine[pl.ds(start, step)].reshape(step * rows, half)
        cut = at(None, start)
        acc_dg[cut, :] = dot(x, dg[0])
        acc_du[cut, :] = dot(x, du[0])
        acc_g[cut, :] = dot(x, eg[0])
        acc_u[cut, :] = dot(x, eu[0])

    chunks(first_half)

    peers(lambda p: send(x_mine.at[p], x_mate.at[p], f_send.at[p], f_recv.at[p], {"tp": mate}).wait_recv())
    for key in (("dg", 1), ("du", 1), ("dd", 0), ("dd", 1)):
        loads[key].wait()
    small[4].wait()

    def dense(start):
        x = x_mate[pl.ds(start, step)].reshape(step * rows, half)
        cut = at(None, start)
        unit = clamped_unit(acc_dg[cut, :] + dot(x, dg[1]), acc_du[cut, :] + dot(x, du[1]))
        hidden[cut, :] = unit
        part = jnp.sum(unit.astype(F32) * gv[...].astype(F32).reshape(1, -1), axis=-1, keepdims=True)
        logit[cut, :] = jnp.broadcast_to(part, (step * rows, extra))
        away = dot(unit, dd[1]).astype(BF16)
        d_give[pl.ds(start, step), :, :half] = away.reshape(step, rows, half)
        lanes = split_lanes(part, (step * rows, extra))
        d_give[pl.ds(start, step), :, half:] = lanes.reshape(step, rows, extra)

    chunks(dense)
    d_pair = send(d_give, d_take, p_send.at[0], p_recv.at[0], {"tp": mate})
    d_pair.start()

    for key in (("eg", 1), ("eu", 1)):
        loads[key].wait()

    def expert(start):
        x = x_mate[pl.ds(start, step)].reshape(step * rows, half)
        cut = at(None, start)
        d_keep[cut, :] = dot(hidden[cut, :], dd[0])
        act[cut, :] = clamped_unit(acc_g[cut, :] + dot(x, eg[1]), acc_u[cut, :] + dot(x, eu[1]))

    chunks(expert)

    d_pair.wait_recv()

    def dense_sum(start):
        cut = at(None, start)
        took = d_take[pl.ds(start, step)].astype(F32).reshape(step * rows, half + extra)
        total = (d_keep[cut, :] + took[:, :half]).astype(BF16)
        d_out[pl.ds(start, step), :, :half] = total.reshape(step, rows, half)
        gate = logit[cut, :][:, :1] + jnp.sum(took[:, half:], axis=-1, keepdims=True)
        lanes = split_lanes(gate, (step * rows, extra))
        d_out[pl.ds(start, step), :, half:] = lanes.reshape(step, rows, extra)

    chunks(dense_sum)
    for key in (("ed", 1), ("ed", 0)):
        loads[key].wait()

    def give(start):
        away = dot(act[at(None, start), :], ed[1]).astype(BF16)
        e_give[pl.ds(start, step)] = away.reshape(step, rows, half)

    chunks(give)
    e_pair = send(e_give, e_take, p_send.at[1], p_recv.at[1], {"tp": mate})
    e_pair.start()
    peers(lambda p: send(d_out.at[p], d_in.at[me], d_send.at[p], d_recv.at[me], {"ep": p}).start())

    def keep(start):
        cut = at(None, start)
        e_keep[cut, :] = dot(act[cut, :], ed[0]).astype(BF16).astype(F32)

    chunks(keep)
    e_pair.wait_recv()

    def expert_sum(start):
        took = e_take[pl.ds(start, step)].astype(F32)
        own = e_keep[at(None, start), :].reshape(step, rows, half)
        e_out[pl.ds(start, step)] = (own + took).astype(BF16)

    chunks(expert_sum)
    peers(lambda p: send(e_out.at[p], e_in.at[me], e_send.at[p], e_recv.at[me], {"ep": p}).start())

    small[2].wait()
    small[3].wait()
    d_in[me] = d_out[me]
    e_in[me] = e_out[me]

    diagonal = lax.broadcasted_iota(jnp.int32, (rows, rows), 0) == lax.broadcasted_iota(
        jnp.int32, (rows, rows), 1
    )

    def column(row):
        return jnp.sum(jnp.where(diagonal, row, 0.0), axis=-1, keepdims=True)

    top = routes.shape[0]
    named = [column(routes[k : k + 1, :].astype(F32)) for k in range(top)]
    factor = [column(weight[k : k + 1, :]) for k in range(top)]

    def scaled(e):
        share = jnp.zeros((rows, 1), F32)
        for k in range(top):
            share = share + jnp.where(named[k] == jnp.asarray(e, F32), factor[k], 0.0)
        return share * e_in[e].astype(F32)

    peers(lambda p: send(d_out.at[p], d_in.at[p], d_send.at[p], d_recv.at[p], {"ep": p}).wait_recv())
    dense_all = jnp.sum(d_in[...].astype(F32), axis=0)
    gate_logit = jnp.sum(dense_all[:, half:], axis=-1, keepdims=True)
    base = jax.nn.sigmoid(gate_logit) * dense_all[:, :half]

    peers(lambda p: send(e_out.at[p], e_in.at[p], e_send.at[p], e_recv.at[p], {"ep": p}).wait_recv())
    if n <= 16:
        mix = scaled(0)
        for e in range(1, n):
            mix = mix + scaled(e)
    else:
        mix = lax.fori_loop(0, n, lambda e, total: total + scaled(e), jnp.zeros((rows, half), F32))
    out_ref[...] = (base + mix).astype(BF16)

    def sent(p):
        send(x_mine.at[me], x_mine.at[me], x_send.at[p], x_recv.at[me], {"ep": p}).wait_send()
        send(x_mine.at[p], x_mate.at[p], f_send.at[p], f_recv.at[p], {"tp": mate}).wait_send()
        send(d_out.at[p], d_in.at[me], d_send.at[p], d_recv.at[me], {"ep": p}).wait_send()
        send(e_out.at[p], e_in.at[me], e_send.at[p], e_recv.at[me], {"ep": p}).wait_send()

    peers(sent)
    d_pair.wait_send()
    e_pair.wait_send()


def solution(mesh):
    n, tp = mesh.shape["ep"], mesh.shape["tp"]
    assert tp == 2

    def per_device(
        tokens, norm_gain, routes, route_weight, expert_gate, expert_up, expert_down,
        dense_gate, dense_up, dense_down, gate_vector,
    ):
        rows, width = tokens.shape
        half = width // tp
        units, wide = expert_gate.shape[2], dense_gate.shape[1]
        step = min(n, 8)
        total = n * rows
        anywhere = pl.BlockSpec(memory_space=pltpu.HBM)
        vmem, dma = pltpu.VMEM, pltpu.SemaphoreType.DMA
        pieces = (n, rows, half)
        wider = (n, rows, half + extra)
        return pl.pallas_call(
            functools.partial(kernel, n, step),
            out_shape=jax.ShapeDtypeStruct((rows, half), BF16),
            in_specs=[anywhere] * 11,
            out_specs=pl.BlockSpec(memory_space=pltpu.VMEM),
            scratch_shapes=[
                vmem((rows, width), BF16), vmem((width,), F32),
                vmem(routes.shape[::-1], jnp.int32), vmem(route_weight.shape[::-1], F32), vmem((wide,), BF16),
                vmem((2, half, units), BF16), vmem((2, half, units), BF16), vmem((2, units, half), BF16),
                vmem((2, half, wide), BF16), vmem((2, half, wide), BF16), vmem((2, wide, half), BF16),
                vmem(pieces, BF16), vmem(pieces, BF16),
                vmem((total, units), F32), vmem((total, units), F32),
                vmem((total, wide), F32), vmem((total, wide), F32),
                vmem((total, units), BF16), vmem((total, wide), BF16),
                vmem((total, half), F32), vmem((total, half), F32), vmem((total, extra), F32),
                vmem(wider, BF16), vmem(wider, BF16), vmem(wider, BF16), vmem(wider, BF16),
                vmem(pieces, BF16), vmem(pieces, BF16), vmem(pieces, BF16), vmem(pieces, BF16),
                dma((5,)), dma((12,)),
                dma((n,)), dma((n,)), dma((n,)), dma((n,)), dma((n,)), dma((n,)), dma((n,)), dma((n,)),
                dma((2,)), dma((2,)),
            ],
            compiler_params=pltpu.CompilerParams(
                collective_id=0, has_side_effects=True, vmem_limit_bytes=vmem_bytes
            ),
        )(
            tokens, norm_gain, routes.T, route_weight.T, expert_gate, expert_up,
            expert_down, dense_gate, dense_up, dense_down, gate_vector,
        )

    in_specs = (
        P(("grp", "ep"), None), P(), P(("grp", "ep"), None), P(("grp", "ep"), None),
        P("ep", None, "tp"), P("ep", None, "tp"), P("ep", "tp", None),
        P(None, ("ep", "tp")), P(None, ("ep", "tp")), P(("ep", "tp"), None), P(("ep", "tp")),
    )
    return jax.shard_map(
        per_device, mesh=mesh, in_specs=in_specs, out_specs=P(("grp", "ep"), "tp"), check_vma=False
    )
```

```python
import functools

import jax
import jax.numpy as jnp
from jax import lax
from jax.experimental import pallas as pl
from jax.experimental.pallas import tpu as pltpu
from jax.sharding import PartitionSpec as P

MESH = pl.DeviceIdType.MESH
F32 = jnp.float32
BF16 = jnp.bfloat16
clamp_limit = 7.0
sigmoid_slope = 1.702
norm_eps = 1e-06
vmem_bytes = 48 * 1024 * 1024
extra = 128


def clamped_unit(gate_pre, up_pre):
    gated = jnp.minimum(gate_pre, clamp_limit)
    linear = jnp.clip(up_pre, -clamp_limit, clamp_limit)
    return (gated * jax.nn.sigmoid(sigmoid_slope * gated) * (linear + 1.0)).astype(BF16)


def split_lanes(value, shape):
    high = value.astype(BF16).astype(F32)
    middle = (value - high).astype(BF16).astype(F32)
    low = value - high - middle
    lane = lax.broadcasted_iota(jnp.int32, shape, len(shape) - 1)
    zero = jnp.zeros(shape, F32)
    out = jnp.where(lane == 0, high, jnp.where(lane == 1, middle, jnp.where(lane == 2, low, zero)))
    return out.astype(BF16)


def kernel(
    n, step,
    tok_hbm, gain_hbm, routes_hbm, weight_hbm, eg_hbm, eu_hbm, ed_hbm, dg_hbm, du_hbm, dd_hbm, gv_hbm,
    out_ref,
    tok, gain, routes, weight, gv, eg, eu, ed, dg, du, dd,
    x_mine, x_mate, acc_g, acc_u, acc_dg, acc_du, act, hidden, d_keep, e_keep, logit,
    d_give, d_take, d_out, d_in, e_give, e_take, e_out, e_in,
    small_sem, load_sem, x_send, x_recv, f_send, f_recv, d_send, d_recv, e_send, e_recv, p_send, p_recv,
):
    me, core = lax.axis_index("ep"), lax.axis_index("tp")
    mate = 1 - core
    rows, half = tok.shape[0], x_mine.shape[2]

    offsets = list(range(1, n))

    def peers(body):
        if n <= 16:
            for off in offsets:
                body(lax.rem(me + off, n))
        else:
            def one(off, carry):
                body(lax.rem(me + off, n))
                return carry
            lax.fori_loop(1, n, one, 0)

    def chunks(body):
        if step == n:
            body(0)
        else:
            def one(index, carry):
                body(index * step)
                return carry
            lax.fori_loop(0, n // step, one, 0)

    def send(src, dst, ssem, rsem, device):
        return pltpu.make_async_remote_copy(
            src_ref=src, dst_ref=dst, send_sem=ssem, recv_sem=rsem,
            device_id=device, device_id_type=MESH,
        )

    barrier = pltpu.get_barrier_semaphore()
    peers(lambda p: pl.semaphore_signal(barrier, inc=1, device_id={"ep": p}, device_id_type=MESH))
    pl.semaphore_signal(barrier, inc=1, device_id={"tp": mate}, device_id_type=MESH)

    small = [
        pltpu.make_async_copy(src, dst, small_sem.at[i])
        for i, (src, dst) in enumerate(
            ((tok_hbm, tok), (gain_hbm, gain), (routes_hbm, routes), (weight_hbm, weight), (gv_hbm, gv))
        )
    ]
    for copy in small:
        copy.start()
    sides = (core, mate)
    loads = {}
    count = 0
    for name, src, dst, along in (
        ("dg", dg_hbm, dg, 0), ("du", du_hbm, du, 0), ("eg", eg_hbm.at[0], eg, 0),
        ("eu", eu_hbm.at[0], eu, 0), ("dd", dd_hbm, dd, 1), ("ed", ed_hbm.at[0], ed, 1),
    ):
        for k in range(2):
            cut = pl.ds(pl.multiple_of(sides[k] * half, 128), half)
            part = src.at[cut, :] if along == 0 else src.at[:, cut]
            loads[name, k] = pltpu.make_async_copy(part, dst.at[k], load_sem.at[count])
            count += 1
    for key in (("dg", 0), ("du", 0), ("eg", 0), ("eu", 0), ("dg", 1), ("du", 1), ("dd", 1), ("dd", 0),
                ("eg", 1), ("eu", 1), ("ed", 1), ("ed", 0)):
        loads[key].start()

    small[0].wait()
    small[1].wait()
    values = tok[...].astype(F32)
    inverse = lax.rsqrt(jnp.mean(values * values, axis=-1, keepdims=True) + norm_eps)
    normed = values * inverse * gain[...].reshape(1, 2 * half)
    left, right = normed[:, :half], normed[:, half:]
    first = core == 0
    x_mine[me] = jnp.where(first, left, right).astype(BF16)
    x_mate[me] = jnp.where(first, right, left).astype(BF16)

    pl.semaphore_wait(barrier, n)
    peers(lambda p: send(x_mine.at[me], x_mine.at[me], x_send.at[p], x_recv.at[me], {"ep": p}).start())

    def forward(p):
        send(x_mine.at[p], x_mine.at[p], x_send.at[p], x_recv.at[p], {"ep": p}).wait_recv()
        send(x_mine.at[p], x_mate.at[p], f_send.at[p], f_recv.at[p], {"tp": mate}).start()

    peers(forward)

    def at(ref, start):
        return pl.ds(start * rows, step * rows)

    def dot(a, b):
        return jnp.dot(a, b, preferred_element_type=F32)

    for key in (("dg", 0), ("du", 0), ("eg", 0), ("eu", 0)):
        loads[key].wait()

    def first_half(start):
        x = x_mine[pl.ds(start, step)].reshape(step * rows, half)
        cut = at(None, start)
        acc_dg[cut, :] = dot(x, dg[0])
        acc_du[cut, :] = dot(x, du[0])
        acc_g[cut, :] = dot(x, eg[0])
        acc_u[cut, :] = dot(x, eu[0])

    chunks(first_half)

    peers(lambda p: send(x_mine.at[p], x_mate.at[p], f_send.at[p], f_recv.at[p], {"tp": mate}).wait_recv())
    for key in (("dg", 1), ("du", 1), ("dd", 0), ("dd", 1)):
        loads[key].wait()
    small[4].wait()

    def dense(start):
        x = x_mate[pl.ds(start, step)].reshape(step * rows, half)
        cut = at(None, start)
        unit = clamped_unit(acc_dg[cut, :] + dot(x, dg[1]), acc_du[cut, :] + dot(x, du[1]))
        hidden[cut, :] = unit
        part = jnp.sum(unit.astype(F32) * gv[...].astype(F32).reshape(1, -1), axis=-1, keepdims=True)
        logit[cut, :] = jnp.broadcast_to(part, (step * rows, extra))
        away = dot(unit, dd[1]).astype(BF16)
        d_give[pl.ds(start, step), :, :half] = away.reshape(step, rows, half)
        lanes = split_lanes(part, (step * rows, extra))
        d_give[pl.ds(start, step), :, half:] = lanes.reshape(step, rows, extra)

    chunks(dense)
    d_pair = send(d_give, d_take, p_send.at[0], p_recv.at[0], {"tp": mate})
    d_pair.start()

    for key in (("eg", 1), ("eu", 1)):
        loads[key].wait()

    def expert(start):
        x = x_mate[pl.ds(start, step)].reshape(step * rows, half)
        cut = at(None, start)
        d_keep[cut, :] = dot(hidden[cut, :], dd[0])
        act[cut, :] = clamped_unit(acc_g[cut, :] + dot(x, eg[1]), acc_u[cut, :] + dot(x, eu[1]))

    chunks(expert)

    d_pair.wait_recv()

    def dense_sum(start):
        cut = at(None, start)
        took = d_take[pl.ds(start, step)].astype(F32).reshape(step * rows, half + extra)
        total = (d_keep[cut, :] + took[:, :half]).astype(BF16)
        d_out[pl.ds(start, step), :, :half] = total.reshape(step, rows, half)
        gate = logit[cut, :][:, :1] + jnp.sum(took[:, half:], axis=-1, keepdims=True)
        lanes = split_lanes(gate, (step * rows, extra))
        d_out[pl.ds(start, step), :, half:] = lanes.reshape(step, rows, extra)

    chunks(dense_sum)
    peers(lambda p: send(d_out.at[p], d_in.at[me], d_send.at[p], d_recv.at[me], {"ep": p}).start())
    for key in (("ed", 1), ("ed", 0)):
        loads[key].wait()

    def give(start):
        away = dot(act[at(None, start), :], ed[1]).astype(BF16)
        e_give[pl.ds(start, step)] = away.reshape(step, rows, half)

    chunks(give)
    e_pair = send(e_give, e_take, p_send.at[1], p_recv.at[1], {"tp": mate})
    e_pair.start()

    def keep(start):
        cut = at(None, start)
        e_keep[cut, :] = dot(act[cut, :], ed[0]).astype(BF16).astype(F32)

    chunks(keep)
    e_pair.wait_recv()

    def expert_sum(start):
        took = e_take[pl.ds(start, step)].astype(F32)
        own = e_keep[at(None, start), :].reshape(step, rows, half)
        e_out[pl.ds(start, step)] = (own + took).astype(BF16)

    chunks(expert_sum)
    peers(lambda p: send(e_out.at[p], e_in.at[me], e_send.at[p], e_recv.at[me], {"ep": p}).start())

    small[2].wait()
    small[3].wait()
    d_in[me] = d_out[me]
    e_in[me] = e_out[me]

    diagonal = lax.broadcasted_iota(jnp.int32, (rows, rows), 0) == lax.broadcasted_iota(
        jnp.int32, (rows, rows), 1
    )

    def column(row):
        return jnp.sum(jnp.where(diagonal, row, 0.0), axis=-1, keepdims=True)

    top = routes.shape[0]
    named = [column(routes[k : k + 1, :].astype(F32)) for k in range(top)]
    factor = [column(weight[k : k + 1, :]) for k in range(top)]

    def scaled(e):
        share = jnp.zeros((rows, 1), F32)
        for k in range(top):
            share = share + jnp.where(named[k] == jnp.asarray(e, F32), factor[k], 0.0)
        return share * e_in[e].astype(F32)

    peers(lambda p: send(d_out.at[p], d_in.at[p], d_send.at[p], d_recv.at[p], {"ep": p}).wait_recv())
    dense_all = jnp.sum(d_in[...].astype(F32), axis=0)
    gate_logit = jnp.sum(dense_all[:, half:], axis=-1, keepdims=True)
    base = jax.nn.sigmoid(gate_logit) * dense_all[:, :half]

    def sent(p):
        send(x_mine.at[me], x_mine.at[me], x_send.at[p], x_recv.at[me], {"ep": p}).wait_send()
        send(x_mine.at[p], x_mate.at[p], f_send.at[p], f_recv.at[p], {"tp": mate}).wait_send()
        send(d_out.at[p], d_in.at[me], d_send.at[p], d_recv.at[me], {"ep": p}).wait_send()

    peers(sent)
    d_pair.wait_send()
    e_pair.wait_send()

    def arrived(p):
        send(e_out.at[p], e_in.at[p], e_send.at[p], e_recv.at[p], {"ep": p}).wait_recv()

    if n <= 16:
        mix = base + scaled(me)
        for off in offsets:
            p = lax.rem(me + off, n)
            arrived(p)
            mix = mix + scaled(p)
    else:
        peers(arrived)
        mix = lax.fori_loop(0, n, lambda e, total: total + scaled(e), base)
    out_ref[...] = mix.astype(BF16)
    peers(lambda p: send(e_out.at[p], e_in.at[me], e_send.at[p], e_recv.at[me], {"ep": p}).wait_send())


def solution(mesh):
    n, tp = mesh.shape["ep"], mesh.shape["tp"]
    assert tp == 2

    def per_device(
        tokens, norm_gain, routes, route_weight, expert_gate, expert_up, expert_down,
        dense_gate, dense_up, dense_down, gate_vector,
    ):
        rows, width = tokens.shape
        half = width // tp
        units, wide = expert_gate.shape[2], dense_gate.shape[1]
        step = min(n, 8)
        total = n * rows
        anywhere = pl.BlockSpec(memory_space=pltpu.HBM)
        vmem, dma = pltpu.VMEM, pltpu.SemaphoreType.DMA
        pieces = (n, rows, half)
        wider = (n, rows, half + extra)
        return pl.pallas_call(
            functools.partial(kernel, n, step),
            out_shape=jax.ShapeDtypeStruct((rows, half), BF16),
            in_specs=[anywhere] * 11,
            out_specs=pl.BlockSpec(memory_space=pltpu.VMEM),
            scratch_shapes=[
                vmem((rows, width), BF16), vmem((width,), F32),
                vmem(routes.shape[::-1], jnp.int32), vmem(route_weight.shape[::-1], F32), vmem((wide,), BF16),
                vmem((2, half, units), BF16), vmem((2, half, units), BF16), vmem((2, units, half), BF16),
                vmem((2, half, wide), BF16), vmem((2, half, wide), BF16), vmem((2, wide, half), BF16),
                vmem(pieces, BF16), vmem(pieces, BF16),
                vmem((total, units), F32), vmem((total, units), F32),
                vmem((total, wide), F32), vmem((total, wide), F32),
                vmem((total, units), BF16), vmem((total, wide), BF16),
                vmem((total, half), F32), vmem((total, half), F32), vmem((total, extra), F32),
                vmem(wider, BF16), vmem(wider, BF16), vmem(wider, BF16), vmem(wider, BF16),
                vmem(pieces, BF16), vmem(pieces, BF16), vmem(pieces, BF16), vmem(pieces, BF16),
                dma((5,)), dma((12,)),
                dma((n,)), dma((n,)), dma((n,)), dma((n,)), dma((n,)), dma((n,)), dma((n,)), dma((n,)),
                dma((2,)), dma((2,)),
            ],
            compiler_params=pltpu.CompilerParams(
                collective_id=0, has_side_effects=True, vmem_limit_bytes=vmem_bytes
            ),
        )(*[pltpu.with_memory_space_constraint(x, pltpu.HBM) for x in (
            tokens, norm_gain, routes.T, route_weight.T, expert_gate, expert_up,
            expert_down, dense_gate, dense_up, dense_down, gate_vector,
        )])

    in_specs = (
        P(("grp", "ep"), None), P(), P(("grp", "ep"), None), P(("grp", "ep"), None),
        P("ep", None, "tp"), P("ep", None, "tp"), P("ep", "tp", None),
        P(None, ("ep", "tp")), P(None, ("ep", "tp")), P(("ep", "tp"), None), P(("ep", "tp")),
    )
    return jax.shard_map(
        per_device, mesh=mesh, in_specs=in_specs, out_specs=P(("grp", "ep"), "tp"), check_vma=False
    )
```

```python
import functools

import jax
import jax.numpy as jnp
from jax import lax
from jax.experimental import pallas as pl
from jax.experimental.pallas import tpu as pltpu
from jax.sharding import PartitionSpec as P

MESH = pl.DeviceIdType.MESH
F32 = jnp.float32
BF16 = jnp.bfloat16
clamp_limit = 7.0
sigmoid_slope = 1.702
norm_eps = 1e-06
vmem_bytes = 48 * 1024 * 1024


def clamped_unit(gate_pre, up_pre):
    gated = jnp.minimum(gate_pre, clamp_limit)
    linear = jnp.clip(up_pre, -clamp_limit, clamp_limit)
    return (gated * jax.nn.sigmoid(sigmoid_slope * gated) * (linear + 1.0)).astype(BF16)


def kernel(
    n, step,
    tok_hbm, gain_hbm, routes_hbm, weight_hbm, eg_hbm, eu_hbm, ed_hbm, dg_hbm, du_hbm, dd_hbm, gv_hbm,
    out_ref,
    tok, gain, routes, weight, gv, eg, eu, ed, dg, du, dd,
    x_mine, x_mate, acc_g, acc_u, acc_dg, acc_du, act, hidden, d_keep, e_keep, l_give, l_take, l_out, l_in,
    d_give, d_take, d_out, d_in, e_give, e_take, e_out, e_in,
    small_sem, load_sem, x_send, x_recv, f_send, f_recv, d_send, d_recv, e_send, e_recv, p_send, p_recv,
    l_send, l_recv,
):
    me, core = lax.axis_index("ep"), lax.axis_index("tp")
    mate = 1 - core
    rows, half = tok.shape[0], x_mine.shape[2]

    paired = n % 2 == 0 and n <= 8
    line = n // 2
    place, side = me // 2, lax.rem(me, 2)
    buddy = me + 1 - 2 * side

    def nearby(k):
        low = k + jnp.where(k >= place, 1, 0)
        top = line - 1 - k
        high = top - jnp.where(top <= place, 1, 0)
        return jnp.where(2 * place < line, low, high)

    def peers(body, far_first=False):
        if paired:
            order = [buddy]
            for k in range(line - 1):
                other = nearby(k)
                order += [2 * other + side, 2 * other + 1 - side]
            for p in order[::-1] if far_first else order:
                body(p)
        else:
            def one(off, carry):
                body(lax.rem(me + off, n))
                return carry
            lax.fori_loop(1, n, one, 0)

    def chunks(body):
        if step == n:
            body(0)
        else:
            def one(index, carry):
                body(index * step)
                return carry
            lax.fori_loop(0, n // step, one, 0)

    def send(src, dst, ssem, rsem, device):
        return pltpu.make_async_remote_copy(
            src_ref=src, dst_ref=dst, send_sem=ssem, recv_sem=rsem,
            device_id=device, device_id_type=MESH,
        )

    barrier = pltpu.get_barrier_semaphore()
    def tell(sem, p):
        pl.semaphore_signal(sem, inc=1, device_id={"ep": p}, device_id_type=MESH)

    pl.semaphore_signal(barrier, inc=1, device_id={"tp": mate}, device_id_type=MESH)
    peers(lambda p: tell(barrier, p))

    small = [
        pltpu.make_async_copy(src, dst, small_sem.at[i])
        for i, (src, dst) in enumerate(
            ((tok_hbm, tok), (gain_hbm, gain), (routes_hbm, routes), (weight_hbm, weight), (gv_hbm, gv))
        )
    ]
    for copy in small:
        copy.start()
    sides = (core, mate)
    loads = {}
    count = 0
    for name, src, dst, along in (
        ("dg", dg_hbm, dg, 0), ("du", du_hbm, du, 0), ("eg", eg_hbm.at[0], eg, 0),
        ("eu", eu_hbm.at[0], eu, 0), ("dd", dd_hbm, dd, 1), ("ed", ed_hbm.at[0], ed, 1),
    ):
        for k in range(2):
            cut = pl.ds(pl.multiple_of(sides[k] * half, 128), half)
            part = src.at[cut, :] if along == 0 else src.at[:, cut]
            loads[name, k] = pltpu.make_async_copy(part, dst.at[k], load_sem.at[count])
            count += 1
    for key in (("dg", 0), ("du", 0), ("eg", 0), ("eu", 0)):
        loads[key].start()

    small[0].wait()
    small[1].wait()
    values = tok[...].astype(F32)
    inverse = lax.rsqrt(jnp.mean(values * values, axis=-1, keepdims=True) + norm_eps)
    normed = values * inverse * gain[...].reshape(1, 2 * half)
    left, right = normed[:, :half], normed[:, half:]
    first = core == 0
    x_mine[me] = jnp.where(first, left, right).astype(BF16)
    x_mate[me] = jnp.where(first, right, left).astype(BF16)

    def to_peer(p, source):
        return send(x_mine.at[source], x_mine.at[source], x_send.at[p], x_recv.at[source], {"ep": p})

    def peer_on(p):
        return send(x_mine.at[p], x_mate.at[p], f_send.at[p], f_recv.at[p], {"tp": mate})

    pl.semaphore_wait(barrier, n)
    peers(lambda p: to_peer(p, me).start(), True)
    for key in (("dg", 1), ("du", 1), ("dd", 1), ("dd", 0), ("eg", 1), ("eu", 1), ("ed", 1), ("ed", 0)):
        loads[key].start()

    def forward(p):
        to_peer(p, p).wait_recv()
        peer_on(p).start()

    peers(forward)

    def at(ref, start):
        return pl.ds(start * rows, step * rows)

    def dot(a, b):
        return jnp.dot(a, b, preferred_element_type=F32)

    for key in (("dg", 0), ("du", 0), ("eg", 0), ("eu", 0)):
        loads[key].wait()

    def first_half(start):
        x = x_mine[pl.ds(start, step)].reshape(step * rows, half)
        cut = at(None, start)
        acc_dg[cut, :] = dot(x, dg[0])
        acc_du[cut, :] = dot(x, du[0])
        acc_g[cut, :] = dot(x, eg[0])
        acc_u[cut, :] = dot(x, eu[0])

    chunks(first_half)

    peers(lambda p: peer_on(p).wait_recv())
    for key in (("dg", 1), ("du", 1), ("dd", 0), ("dd", 1)):
        loads[key].wait()
    small[4].wait()

    def dense(start):
        x = x_mate[pl.ds(start, step)].reshape(step * rows, half)
        cut = at(None, start)
        unit = clamped_unit(acc_dg[cut, :] + dot(x, dg[1]), acc_du[cut, :] + dot(x, du[1]))
        hidden[cut, :] = unit
        vector = jnp.broadcast_to(gv[...].astype(F32).reshape(1, -1), (8, unit.shape[1])).astype(BF16)
        logits = lax.dot_general(vector, unit, (((1,), (1,)), ((), ())), preferred_element_type=F32)
        l_give[:, pl.ds(pl.multiple_of(start * rows, step * rows), step * rows)] = logits[:1]
        away = dot(unit, dd[1]).astype(BF16)
        d_give[pl.ds(start, step)] = away.reshape(step, rows, half)

    chunks(dense)
    d_pair = send(d_give, d_take, p_send.at[0], p_recv.at[0], {"tp": mate})
    d_pair.start()
    l_pair = send(l_give, l_take, p_send.at[2], p_recv.at[2], {"tp": mate})
    l_pair.start()

    for key in (("eg", 1), ("eu", 1)):
        loads[key].wait()

    def expert(start):
        x = x_mate[pl.ds(start, step)].reshape(step * rows, half)
        cut = at(None, start)
        d_keep[cut, :] = dot(hidden[cut, :], dd[0])
        act[cut, :] = clamped_unit(acc_g[cut, :] + dot(x, eg[1]), acc_u[cut, :] + dot(x, eu[1]))

    chunks(expert)

    d_pair.wait_recv()
    l_pair.wait_recv()
    l_out[...] = l_give[...] + l_take[...]

    def dense_sum(start):
        cut = at(None, start)
        took = d_take[pl.ds(start, step)].astype(F32).reshape(step * rows, half)
        total = (d_keep[cut, :] + took).astype(BF16)
        d_out[pl.ds(start, step)] = total.reshape(step, rows, half)

    chunks(dense_sum)
    peers(lambda p: send(l_out, l_in.at[me], l_send.at[p], l_recv.at[me], {"ep": p}).start(), True)
    peers(lambda p: send(d_out.at[p], d_in.at[me], d_send.at[p], d_recv.at[me], {"ep": p}).start(), True)
    for key in (("ed", 1), ("ed", 0)):
        loads[key].wait()

    def give(start):
        away = dot(act[at(None, start), :], ed[1]).astype(BF16)
        e_give[pl.ds(start, step)] = away.reshape(step, rows, half)

    chunks(give)
    e_pair = send(e_give, e_take, p_send.at[1], p_recv.at[1], {"tp": mate})
    e_pair.start()

    def keep(start):
        cut = at(None, start)
        e_keep[cut, :] = dot(act[cut, :], ed[0]).astype(BF16).astype(F32)

    chunks(keep)
    e_pair.wait_recv()

    def expert_sum(start):
        took = e_take[pl.ds(start, step)].astype(F32)
        own = e_keep[at(None, start), :].reshape(step, rows, half)
        e_out[pl.ds(start, step)] = (own + took).astype(BF16)

    chunks(expert_sum)
    peers(lambda p: send(e_out.at[p], e_in.at[me], e_send.at[p], e_recv.at[me], {"ep": p}).start(), True)

    small[2].wait()
    small[3].wait()
    d_in[me] = d_out[me]
    l_in[me] = l_out[...]
    e_in[me] = e_out[me]

    diagonal = lax.broadcasted_iota(jnp.int32, (rows, rows), 0) == lax.broadcasted_iota(
        jnp.int32, (rows, rows), 1
    )

    def column(row):
        return jnp.sum(jnp.where(diagonal, row, 0.0), axis=-1, keepdims=True)

    top = routes.shape[0]
    named = [column(routes[k : k + 1, :].astype(F32)) for k in range(top)]
    factor = [column(weight[k : k + 1, :]) for k in range(top)]

    def scaled(e):
        share = jnp.zeros((rows, 1), F32)
        for k in range(top):
            share = share + jnp.where(named[k] == jnp.asarray(e, F32), factor[k], 0.0)
        return share * e_in[e].astype(F32)

    peers(lambda p: send(l_out, l_in.at[p], l_send.at[p], l_recv.at[p], {"ep": p}).wait_recv())
    peers(lambda p: send(d_out.at[p], d_in.at[p], d_send.at[p], d_recv.at[p], {"ep": p}).wait_recv())
    dense_all = jnp.sum(d_in[...].astype(F32), axis=0)
    every = jnp.sum(l_in[...], axis=0)
    spot = (rows, every.shape[1])
    mine = lax.broadcasted_iota(jnp.int32, spot, 1) == me * rows + lax.broadcasted_iota(jnp.int32, spot, 0)
    gate_logit = jnp.sum(jnp.where(mine, every, 0.0), axis=-1, keepdims=True)
    base = jax.nn.sigmoid(gate_logit) * dense_all

    def gathered(p):
        to_peer(p, me).wait_send()
        peer_on(p).wait_send()

    peers(gathered)

    def sent(p):
        send(l_out, l_in.at[me], l_send.at[p], l_recv.at[me], {"ep": p}).wait_send()
        send(d_out.at[p], d_in.at[me], d_send.at[p], d_recv.at[me], {"ep": p}).wait_send()

    peers(sent)
    d_pair.wait_send()
    l_pair.wait_send()
    e_pair.wait_send()

    def arrived(p):
        send(e_out.at[p], e_in.at[p], e_send.at[p], e_recv.at[p], {"ep": p}).wait_recv()

    if paired:
        mix = base + scaled(me)
        order = []
        peers(order.append)
        for p in order:
            arrived(p)
            mix = mix + scaled(p)
    else:
        peers(arrived)
        mix = lax.fori_loop(0, n, lambda e, total: total + scaled(e), base)
    out_ref[...] = mix.astype(BF16)
    peers(lambda p: send(e_out.at[p], e_in.at[me], e_send.at[p], e_recv.at[me], {"ep": p}).wait_send())


def solution(mesh):
    n, tp = mesh.shape["ep"], mesh.shape["tp"]
    assert tp == 2

    def per_device(
        tokens, norm_gain, routes, route_weight, expert_gate, expert_up, expert_down,
        dense_gate, dense_up, dense_down, gate_vector,
    ):
        rows, width = tokens.shape
        half = width // tp
        units, wide = expert_gate.shape[2], dense_gate.shape[1]
        step = n if n <= 8 else 16
        total = n * rows
        anywhere = pl.BlockSpec(memory_space=pltpu.HBM)
        vmem, dma = pltpu.VMEM, pltpu.SemaphoreType.DMA
        pieces = (n, rows, half)
        return pl.pallas_call(
            functools.partial(kernel, n, step),
            out_shape=jax.ShapeDtypeStruct((rows, half), BF16),
            in_specs=[anywhere] * 11,
            out_specs=pl.BlockSpec(memory_space=pltpu.VMEM),
            scratch_shapes=[
                vmem((rows, width), BF16), vmem((width,), F32),
                vmem(routes.shape[::-1], jnp.int32), vmem(route_weight.shape[::-1], F32), vmem((wide,), BF16),
                vmem((2, half, units), BF16), vmem((2, half, units), BF16), vmem((2, units, half), BF16),
                vmem((2, half, wide), BF16), vmem((2, half, wide), BF16), vmem((2, wide, half), BF16),
                vmem(pieces, BF16), vmem(pieces, BF16),
                vmem((total, units), F32), vmem((total, units), F32),
                vmem((total, wide), F32), vmem((total, wide), F32),
                vmem((total, units), BF16), vmem((total, wide), BF16),
                vmem((total, half), F32), vmem((total, half), F32), vmem((1, total), F32), vmem((1, total), F32), vmem((1, total), F32), vmem((n, 1, total), F32),
                vmem(pieces, BF16), vmem(pieces, BF16), vmem(pieces, BF16), vmem(pieces, BF16),
                vmem(pieces, BF16), vmem(pieces, BF16), vmem(pieces, BF16), vmem(pieces, BF16),
                dma((5,)), dma((12,)),
                dma((n,)), dma((n,)), dma((n,)), dma((n,)), dma((n,)), dma((n,)), dma((n,)), dma((n,)),
                dma((3,)), dma((3,)),
                dma((n,)), dma((n,)),
            ],
            compiler_params=pltpu.CompilerParams(
                collective_id=0, has_side_effects=True, vmem_limit_bytes=vmem_bytes
            ),
        )(*[pltpu.with_memory_space_constraint(x, pltpu.HBM) for x in (
            tokens, norm_gain, routes.T, route_weight.T, expert_gate, expert_up,
            expert_down, dense_gate, dense_up, dense_down, gate_vector,
        )])

    in_specs = (
        P(("grp", "ep"), None), P(), P(("grp", "ep"), None), P(("grp", "ep"), None),
        P("ep", None, "tp"), P("ep", None, "tp"), P("ep", "tp", None),
        P(None, ("ep", "tp")), P(None, ("ep", "tp")), P(("ep", "tp"), None), P(("ep", "tp")),
    )
    return jax.shard_map(
        per_device, mesh=mesh, in_specs=in_specs, out_specs=P(("grp", "ep"), "tp"), check_vma=False
    )
```
